32 devices in a mesh: ep: 8 (over z, x), tp: 4 (over y, core).
Axes of the slice: x: 2, y: 2, z: 4, core: 2. Of those that a mesh axis runs over, the one named last changes fastest.
Arguments:
- conv_gate: bfloat16 [4096, 2048], P('ep', 'tp'), may hold values from -6 to 6
- conv_in_gate: bfloat16 [4096, 2048], P('ep', 'tp'), may hold values from -6 to 6
- conv_value: bfloat16 [4096, 2048], P('ep', 'tp'), may hold values from -6 to 6
- conv_taps: float32 [3, 2048], P(None, 'tp'), may hold values from -3.5 to 3.5
- mix_out_weight: bfloat16 [2048, 4096], P(None, 'tp'), may hold values from -0.125 to 0.125
- expert_input: bfloat16 [1280, 4096], P('ep', 'tp'), may hold values from -1600 to 1600
- expert_gain: float32 [4096], replicated, may hold values from 0.1 to 1.9
- routes: int32 [1280, 2], P('ep'), may hold values from 0 to 7, all different within a row; in each aligned block of 160 rows (0 to 159, 160 to 319, ...) at most 60 rows name the same one
- group_prob: float32 [1280], P('ep'), may hold values from 0.3 to 1
- pair_logits: float32 [1280, 2], P('ep'), may hold values from -6 to 6
- expert_gate: bfloat16 [8, 4096, 2048], P('ep', None, 'tp'), may hold values from -0.09375 to 0.09375
- expert_up: bfloat16 [8, 4096, 2048], P('ep', None, 'tp'), may hold values from -0.09375 to 0.09375
- expert_down: bfloat16 [8, 2048, 4096], P('ep', None, 'tp'), may hold values from -0.125 to 0.125
Outputs:
- mixed: bfloat16 [4096, 4096], P('ep', 'tp')
- expert_output: bfloat16 [1280, 4096], P('ep', 'tp')
The draws below stay inside these ranges and needn't reach their ends.
Inputs may be any that keep to these rules, and one draw needn't show every extreme that they name: `routes`: in the 160 rows of one index of ep no expert is named by more than 60 rows, a bound that some block reaches; each row names 2 different experts.
All inputs are finite; a program needn't handle non-finite values.
Results may differ from the reference program's by a relative error of at most 0.0071.
Values may be sent and summed in bfloat16 or wider, within the bound.
No kernel may reach another device: no remote copies, remote signals or barrier semaphores. Data moves between devices by JAX's collectives and lax.ppermute only.
A program may use at most 64 MiB of HBM per device.

```python
import math
import jax
import jax.numpy as jnp
import numpy as np
from jax import lax

D = 4096
CONV_W = 2048
KERNEL = 3
EXPERT_FF = 2048
TOP = 2
TOK_B_DEV = 160
EXPERTS = 8
CAP = 60
TOK_A = 4096
TOK_B = 1280
N_EP = 8


def draw_expert_input(key, part):
    key_base = jax.random.fold_in(key, 11)
    key_row = jax.random.fold_in(key, 12)
    key_col = jax.random.fold_in(key, 13)
    ramp = jnp.arange(D, dtype=jnp.float32) / D
    base = jnp.clip(jax.random.normal(key_base, (TOK_B, D), jnp.float32), -5.0, 5.0)
    slope = jnp.log(3.0)
    row_scale = 10.0 ** jax.random.uniform(key_row, (TOK_B, 1), jnp.float32)
    col_scale = 10.0 ** jax.random.uniform(key_col, (1, D), jnp.float32) * jnp.exp(slope * ramp)[None, :]
    return (base * row_scale * col_scale).astype(jnp.bfloat16)


def block_levels(stream_key, dims, split, least, high):
    def one(axis_at, blocks):
        heights = jax.random.uniform(jax.random.fold_in(jax.random.fold_in(stream_key, 6), axis_at), (blocks,), jnp.float32, least / len(split), high / len(split))
        return jnp.repeat(jnp.exp(heights), dims[axis_at] // blocks).reshape((-1,) + (1,) * (len(dims) - axis_at - 1))

    factor_of = one(*split[0])
    for cut in split[1:]:
        factor_of = factor_of * one(*cut)
    return factor_of


def routed_block(key, own, number, rows, amount, top, bound, skew):
    order = jax.random.permutation(key, amount)
    packed, common = load_shares(amount, rows * top, bound, skew, True), load_shares(amount, rows * top, bound, skew, False)
    places = jnp.arange(amount)

    def named(lengths, rotation):
        used = int((lengths > 0).sum())
        fixed = max(1, used // 4)
        shifted = fixed + (places - fixed + rotation * (used - fixed)) % max(1, amount - fixed)
        return jnp.zeros((amount,), jnp.int32).at[order[jnp.where(places < fixed, places, shifted)]].set(jnp.asarray(lengths, jnp.int32))

    lengths = jnp.where(number % 4 == 0, named(packed, number // 4), named(common, number - number // 4 - 1))
    mixed = jax.random.permutation(jax.random.fold_in(own, 3), amount)
    giver, receiver = mixed[0:amount // 2 * 2:2], mixed[1:amount // 2 * 2:2]
    margin = jnp.minimum(lengths[giver] - 1, bound - lengths[receiver]) // 2
    margin = jnp.where((giver == order[0]) | (receiver == order[0]) | (lengths[receiver] == 0), 0, jnp.maximum(margin, 0))
    shifted = jax.random.randint(jax.random.fold_in(own, 4), (amount // 2,), 0, 1 << 20) % (margin + 1)
    lengths = lengths.at[giver].add(-shifted).at[receiver].add(shifted)
    items = jnp.searchsorted(jnp.cumsum(lengths), jnp.arange(rows * top), side="right").astype(jnp.int32)
    grid = items.reshape(top, rows).T
    grid = grid[jax.random.permutation(jax.random.fold_in(own, 1), rows)]
    rotation = jax.random.randint(jax.random.fold_in(own, 2), (rows, 1), 0, top)
    return jnp.take_along_axis(grid, (jnp.arange(top)[None, :] + rotation) % top, axis=1)


def load_shares(count, total, most, skew, full):
    portions = [(1 << 20) // math.isqrt(rank ** skew) + 1 for rank in range(1, count + 1)]
    largest = most if full else min(most, max(-(-total // count), total * portions[0] // sum(portions)))
    least = 1 if total - largest >= count - 1 else 0
    counts, rest = [largest] + [least] * (count - 1), total - largest - least * (count - 1)
    while rest > 0:
        free = [i for i in range(1, count) if counts[i] < largest] or [i for i in range(1, count) if counts[i] < most]
        pool, budget = sum([portions[i] for i in free]), rest
        for i in free:
            more = min(most - counts[i], max(1, budget * portions[i] // pool), rest)
            counts[i] = counts[i] + more
            rest = rest - more
    return np.array(counts)


def normal_values(key, dims, width, most, shards=(), held_as=jnp.bfloat16):
    array = jax.random.normal(key, dims, jnp.float32) * width
    if len(shards) > 0:
        array = block_levels(key, dims, shards, -0.22, 0.18) * array
    return jnp.clip(array, min=-most, max=most).astype(held_as)


def setup_inputs(seed: int = 0) -> dict:
    arg_keys = jax.random.split(jax.random.key(seed), 14)
    conv_gate = normal_values(arg_keys[0], (TOK_A, CONV_W), 1.0, 6.0, ((0, 8), (1, 4)))
    conv_in_gate = normal_values(arg_keys[1], (TOK_A, CONV_W), 1.0, 6.0, ((0, 8), (1, 4)))
    conv_value = normal_values(arg_keys[2], (TOK_A, CONV_W), 1.0, 6.0, ((0, 8), (1, 4)))
    conv_taps = normal_values(arg_keys[3], (KERNEL, CONV_W), KERNEL ** -0.5, 3.5, ((1, 4),), jnp.float32)
    mix_out_weight = normal_values(arg_keys[4], (CONV_W, D), CONV_W ** -0.5, 0.125, ((1, 4),))
    expert_input = draw_expert_input(jax.random.fold_in(arg_keys[13], 71), 0)
    expert_gain = jnp.clip(1.0 + 0.18 * jax.random.normal(arg_keys[6], (D,), jnp.float32), 0.1, 1.9)
    routes_keys = jax.random.split(jax.random.fold_in(arg_keys[7], 1), TOK_B // TOK_B_DEV)
    routes_turns = jax.random.permutation(jax.random.fold_in(arg_keys[7], 3), TOK_B // TOK_B_DEV)
    routes = jax.vmap(lambda own, number: routed_block(jax.random.fold_in(arg_keys[7], 2), own, number, TOK_B_DEV, EXPERTS, TOP, CAP, 1))(routes_keys, routes_turns).reshape((TOK_B, TOP))
    group_prob = jnp.clip(0.3 + 0.7 * jax.random.uniform(arg_keys[8], (TOK_B,), jnp.float32) ** block_levels(arg_keys[8], (TOK_B,), ((0, 8),), -0.2, 0.2), 0.3, 1.0)
    pair_logits = normal_values(arg_keys[9], (TOK_B, TOP), 1.5, 6.0, ((0, 8),), jnp.float32)
    expert_gate = normal_values(arg_keys[10], (EXPERTS, D, EXPERT_FF), D ** -0.5, 0.09375, ((0, 8), (2, 4)))
    expert_up = normal_values(arg_keys[11], (EXPERTS, D, EXPERT_FF), D ** -0.5, 0.09375, ((0, 8), (2, 4)))
    expert_down = normal_values(arg_keys[12], (EXPERTS, EXPERT_FF, D), EXPERT_FF ** -0.5, 0.125, ((0, 8), (2, 4)))
    return dict(conv_gate=conv_gate, conv_in_gate=conv_in_gate, conv_value=conv_value, conv_taps=conv_taps, mix_out_weight=mix_out_weight, expert_input=expert_input, expert_gain=expert_gain, routes=routes, group_prob=group_prob, pair_logits=pair_logits, expert_gate=expert_gate, expert_up=expert_up, expert_down=expert_down)


EPS = 1e-06

def slot_table(route_block, capacity, expert_count):
    pair_ids = route_block.reshape(-1)
    onehot = (pair_ids[:, None] == jnp.arange(expert_count, dtype=jnp.int32)[None, :]).astype(jnp.int32)
    earlier = jnp.cumsum(onehot, axis=0) - onehot
    within = lax.optimization_barrier(jnp.sum(earlier * onehot, axis=1))
    return (pair_ids * capacity + within).astype(jnp.int32)

def pair_weights(group_prob, pair_logits):
    spread = pair_logits[:, 0] - pair_logits[:, 1]
    return jnp.stack([jax.nn.sigmoid(spread), jax.nn.sigmoid(-spread)], axis=1) * group_prob[:, None]

def expert_rows(item):
    arrived, gate_w, up_w, down_w = item
    gate_sum = jnp.dot(arrived, gate_w, preferred_element_type=jnp.float32)
    up_sum = jnp.dot(arrived, up_w, preferred_element_type=jnp.float32)
    hidden = (jax.nn.silu(gate_sum) * up_sum).astype(jnp.bfloat16)
    return jnp.dot(hidden, down_w, preferred_element_type=jnp.float32).astype(jnp.bfloat16)

def reference(conv_gate, conv_in_gate, conv_value, conv_taps, mix_out_weight, expert_input, expert_gain, routes, group_prob, pair_logits, expert_gate, expert_up, expert_down):
    products = conv_in_gate.astype(jnp.float32) * conv_value.astype(jnp.float32)
    padded = jnp.concatenate([jnp.zeros((KERNEL - 1, CONV_W), jnp.float32), products], axis=0)
    convolved = jnp.zeros_like(products)
    for offset in range(KERNEL):
        convolved = convolved + conv_taps[offset][None, :] * padded[offset:offset + TOK_A]
    mixer_rows = (conv_gate.astype(jnp.float32) * convolved).astype(jnp.bfloat16)
    mixed = jnp.dot(mixer_rows, mix_out_weight, preferred_element_type=jnp.float32).astype(jnp.bfloat16)
    features = expert_input.astype(jnp.float32)
    scale = lax.rsqrt(lax.optimization_barrier(jnp.mean(features * features, axis=1)) + EPS)
    normed = (features * scale[:, None] * expert_gain[None, :]).astype(jnp.bfloat16)
    blocks = routes.reshape(N_EP, TOK_B_DEV, TOP)

    def block_slots(route_block):
        return slot_table(route_block, CAP, EXPERTS)
    slot_index = jax.vmap(block_slots)(blocks)
    pair_row = (jnp.arange(TOK_B_DEV * TOP, dtype=jnp.int32) // TOP).astype(jnp.int32)
    normed_blocks = normed.reshape(N_EP, TOK_B_DEV, D)

    def fill_buffer(rows_block, slots_block):
        return jnp.zeros((EXPERTS * CAP, D), jnp.bfloat16).at[slots_block].set(rows_block[pair_row])
    buffers = jax.vmap(fill_buffer)(normed_blocks, slot_index)
    per_expert = buffers.reshape(N_EP, EXPERTS, CAP, D).transpose(1, 0, 2, 3).reshape(EXPERTS, N_EP * CAP, D)
    results = lax.map(expert_rows, (per_expert, expert_gate, expert_up, expert_down))
    returned = results.reshape(EXPERTS, N_EP, CAP, D).transpose(1, 0, 2, 3).reshape(N_EP, EXPERTS * CAP, D)

    def pick_rows(table, slots_block):
        return table[slots_block]
    picked = jax.vmap(pick_rows)(returned, slot_index).reshape(TOK_B, TOP, D).astype(jnp.float32)
    weights = pair_weights(group_prob, pair_logits)
    expert_output = lax.optimization_barrier(jnp.sum(picked * weights[:, :, None], axis=1)).astype(jnp.bfloat16)
    return (mixed, expert_output)
```

```python
import jax
import jax.numpy as jnp
from jax import lax
from jax.sharding import PartitionSpec as P

D = 4096
EPS = 1e-06
CHUNKS = 1
PERMUTED = False


def shifted(block, axis, distance):
    devices = range(lax.axis_size(axis))
    route = [(i - distance, i) for i in devices if i - distance in devices]
    return lax.ppermute(block, axis, route)


def rotated(block, axis, distance):
    size = lax.axis_size(axis)
    return lax.ppermute(block, axis, [(i, (i + distance) % size) for i in range(size)])


def core_swapped(block):
    return lax.ppermute(block, "tp", [(i, i ^ 1) for i in range(lax.axis_size("tp"))])


def chip_rotated(block, distance):
    size = lax.axis_size("tp")
    return lax.ppermute(block, "tp", [(i, (i + 2 * distance) % size) for i in range(size)])


def pieces_over_tp(block):
    size = lax.axis_size("tp")
    own = lax.axis_index("tp")
    pieces = [(own, block), (own ^ 1, core_swapped(block))]
    for distance in range(1, size // 2):
        piece = chip_rotated(block, distance)
        source = (own - 2 * distance) % size
        pieces = pieces + [(source, piece), (source ^ 1, core_swapped(piece))]
    return pieces


def rows_of(weight, start, count):
    return lax.dynamic_slice_in_dim(weight, start, count, 0)


def summed_product(pieces, weight):
    total = None
    for source, piece in pieces:
        width = piece.shape[1]
        part = jnp.dot(
            piece, rows_of(weight, source * width, width), preferred_element_type=jnp.float32
        )
        total = part if total is None else total + part
    return total


def pair_weights(group_prob, pair_logits):
    spread = pair_logits[:, 0] - pair_logits[:, 1]
    return (
        jnp.stack([jax.nn.sigmoid(spread), jax.nn.sigmoid(-spread)], axis=1) * group_prob[:, None]
    )


def send_out(buffer, expert_count):
    rows, width = buffer.shape
    capacity = rows // expert_count
    if not PERMUTED:
        return lax.all_to_all(
            buffer.reshape(expert_count, capacity, width), "ep", 0, 0, tiled=True
        ).reshape(rows, width)
    blocks = [buffer[:capacity]]
    for j in range(1, expert_count):
        blocks.append(rotated(buffer[j * capacity : (j + 1) * capacity], "ep", j))
    return jnp.concatenate(blocks, axis=0)


def send_back(buffer, expert_count):
    rows, width = buffer.shape
    capacity = rows // expert_count
    if not PERMUTED:
        return send_out(buffer, expert_count)
    blocks = [buffer[:capacity]]
    for j in range(1, expert_count):
        blocks.append(rotated(buffer[j * capacity : (j + 1) * capacity], "ep", -j))
    return jnp.concatenate(blocks, axis=0)


def per_device(
    conv_gate,
    conv_in_gate,
    conv_value,
    conv_taps,
    mix_out_weight,
    expert_input,
    expert_gain,
    routes,
    group_prob,
    pair_logits,
    expert_gate,
    expert_up,
    expert_down,
):
    reach = conv_taps.shape[0] - 1
    token_rows = conv_value.shape[0]
    expert_count = lax.axis_size("ep")
    tok_rows, choose_count = routes.shape
    capacity = 3 * tok_rows * choose_count // (2 * expert_count)
    capacity = -(-capacity // 8) * 8
    slot_rows = expert_count * capacity

    experts = jnp.arange(expert_count, dtype=jnp.int32)
    if PERMUTED:
        experts = (experts + lax.axis_index("ep")) % expert_count
    member = (routes[:, None, :] == experts[None, :, None]).astype(jnp.float32)
    named = jnp.sum(member, axis=2)
    token = jnp.arange(tok_rows, dtype=jnp.int32)
    before = (token[None, :] < token[:, None]).astype(jnp.bfloat16)
    earlier = jnp.dot(before, named.astype(jnp.bfloat16), preferred_element_type=jnp.float32)
    place = jnp.where(named > 0, earlier, -1.0)
    slot = jnp.arange(capacity, dtype=jnp.int32).astype(jnp.float32)
    chosen = (place.T[:, None, :] == slot[None, :, None]).reshape(slot_rows, tok_rows)
    chosen = chosen.astype(jnp.bfloat16)

    gate_block = expert_gate[0]
    up_block = expert_up[0]
    down_block = expert_down[0]
    columns = expert_input.shape[1]
    span = columns // CHUNKS
    gate_sum = None
    up_sum = None
    squares = None
    for chunk in range(CHUNKS):
        part = expert_input[:, chunk * span : (chunk + 1) * span]
        buffer = jnp.dot(chosen, part, preferred_element_type=jnp.float32).astype(jnp.bfloat16)
        arrived = send_out(buffer, expert_count)
        for source, piece in pieces_over_tp(arrived):
            start = source * columns + chunk * span
            features = piece.astype(jnp.float32)
            piece_squares = jnp.sum(features * features, axis=1)
            gained = (features * rows_of(expert_gain, start, span)[None, :]).astype(jnp.bfloat16)
            gate_part = jnp.dot(
                gained, rows_of(gate_block, start, span), preferred_element_type=jnp.float32
            )
            up_part = jnp.dot(
                gained, rows_of(up_block, start, span), preferred_element_type=jnp.float32
            )
            if squares is None:
                gate_sum, up_sum, squares = gate_part, up_part, piece_squares
            else:
                gate_sum = gate_sum + gate_part
                up_sum = up_sum + up_part
                squares = squares + piece_squares
    scale = lax.rsqrt(squares / D + EPS)[:, None]
    hidden = (jax.nn.silu(gate_sum * scale) * (up_sum * scale)).astype(jnp.bfloat16)
    results = summed_product(pieces_over_tp(hidden), down_block).astype(jnp.bfloat16)
    returned = send_back(results, expert_count)

    products = conv_in_gate.astype(jnp.float32) * conv_value.astype(jnp.float32)
    earlier_rows = shifted(products[token_rows - reach :], "ep", 1)
    padded = jnp.concatenate([earlier_rows, products], axis=0)
    convolved = jnp.zeros_like(products)
    for offset in range(reach + 1):
        convolved = convolved + conv_taps[offset][None, :] * padded[offset : offset + token_rows]
    mixer_rows = (conv_gate.astype(jnp.float32) * convolved).astype(jnp.bfloat16)
    mixed = summed_product(pieces_over_tp(mixer_rows), mix_out_weight).astype(jnp.bfloat16)

    weights = pair_weights(group_prob, pair_logits)
    by_expert = jnp.sum(member * weights[:, None, :], axis=2)
    spread_weights = (
        (place[:, :, None] == slot[None, None, :]).astype(jnp.float32) * by_expert[:, :, None]
    ).reshape(tok_rows, slot_rows)
    high = lax.reduce_precision(spread_weights, 8, 7)
    low = (spread_weights - high).astype(jnp.bfloat16)
    expert_output = (
        jnp.dot(high.astype(jnp.bfloat16), returned, preferred_element_type=jnp.float32)
        + jnp.dot(low, returned, preferred_element_type=jnp.float32)
    ).astype(jnp.bfloat16)
    return (mixed, expert_output)


def solution(mesh):
    in_specs = (
        P("ep", "tp"),
        P("ep", "tp"),
        P("ep", "tp"),
        P(None, "tp"),
        P(None, "tp"),
        P("ep", "tp"),
        P(),
        P("ep", None),
        P("ep"),
        P("ep", None),
        P("ep", None, "tp"),
        P("ep", None, "tp"),
        P("ep", None, "tp"),
    )
    out_specs = (P("ep", "tp"), P("ep", "tp"))
    return jax.shard_map(
        per_device, mesh=mesh, in_specs=in_specs, out_specs=out_specs, check_vma=False
    )
```

```python
import jax
import jax.numpy as jnp
from jax import lax
from jax.sharding import PartitionSpec as P

D = 4096
EPS = 1e-06
PERMUTED = False


def shifted(block, axis, distance):
    devices = range(lax.axis_size(axis))
    route = [(i - distance, i) for i in devices if i - distance in devices]
    return lax.ppermute(block, axis, route)


def rotated(block, axis, distance):
    size = lax.axis_size(axis)
    return lax.ppermute(block, axis, [(i, (i + distance) % size) for i in range(size)])


def core_swapped(block):
    return lax.ppermute(block, "tp", [(i, i ^ 1) for i in range(lax.axis_size("tp"))])


def chip_rotated(block, distance):
    size = lax.axis_size("tp")
    return lax.ppermute(block, "tp", [(i, (i + 2 * distance) % size) for i in range(size)])


def pieces_over_tp(block):
    size = lax.axis_size("tp")
    own = lax.axis_index("tp")
    pieces = [(own, block), (own ^ 1, core_swapped(block))]
    for distance in range(1, size // 2):
        piece = chip_rotated(block, distance)
        source = (own - 2 * distance) % size
        pieces = pieces + [(source, piece), (source ^ 1, core_swapped(piece))]
    return pieces


def rows_of(weight, start, count):
    return lax.dynamic_slice_in_dim(weight, start, count, 0)


def summed_product(pieces, weight):
    total = None
    for source, piece in pieces:
        width = piece.shape[1]
        part = jnp.dot(
            piece, rows_of(weight, source * width, width), preferred_element_type=jnp.float32
        )
        total = part if total is None else total + part
    return total


def pair_weights(group_prob, pair_logits):
    spread = pair_logits[:, 0] - pair_logits[:, 1]
    return (
        jnp.stack([jax.nn.sigmoid(spread), jax.nn.sigmoid(-spread)], axis=1) * group_prob[:, None]
    )


def send_out(buffer, expert_count):
    rows, width = buffer.shape
    capacity = rows // expert_count
    if not PERMUTED:
        return lax.all_to_all(
            buffer.reshape(expert_count, capacity, width), "ep", 0, 0, tiled=True
        ).reshape(rows, width)
    blocks = [buffer[:capacity]]
    for j in range(1, expert_count):
        blocks.append(rotated(buffer[j * capacity : (j + 1) * capacity], "ep", j))
    return jnp.concatenate(blocks, axis=0)


def send_back(buffer, expert_count):
    rows, width = buffer.shape
    capacity = rows // expert_count
    if not PERMUTED:
        return send_out(buffer, expert_count)
    blocks = [buffer[:capacity]]
    for j in range(1, expert_count):
        blocks.append(rotated(buffer[j * capacity : (j + 1) * capacity], "ep", -j))
    return jnp.concatenate(blocks, axis=0)


def per_device(
    conv_gate,
    conv_in_gate,
    conv_value,
    conv_taps,
    mix_out_weight,
    expert_input,
    expert_gain,
    routes,
    group_prob,
    pair_logits,
    expert_gate,
    expert_up,
    expert_down,
):
    reach = conv_taps.shape[0] - 1
    token_rows = conv_value.shape[0]
    expert_count = lax.axis_size("ep")
    tok_rows, choose_count = routes.shape
    capacity = 3 * tok_rows * choose_count // (2 * expert_count)
    capacity = -(-capacity // 8) * 8
    slot_rows = expert_count * capacity

    experts = jnp.arange(expert_count, dtype=jnp.int32)
    if PERMUTED:
        experts = (experts + lax.axis_index("ep")) % expert_count
    member = (routes[:, None, :] == experts[None, :, None]).astype(jnp.float32)
    named = jnp.sum(member, axis=2)
    token = jnp.arange(tok_rows, dtype=jnp.int32)
    before = (token[None, :] < token[:, None]).astype(jnp.bfloat16)
    earlier = jnp.dot(before, named.astype(jnp.bfloat16), preferred_element_type=jnp.float32)
    place = jnp.where(named > 0, earlier, -1.0)
    slot = jnp.arange(capacity, dtype=jnp.int32).astype(jnp.float32)
    chosen = (place.T[:, None, :] == slot[None, :, None]).reshape(slot_rows, tok_rows)
    chosen = chosen.astype(jnp.bfloat16)

    gate_block = expert_gate[0]
    up_block = expert_up[0]
    down_block = expert_down[0]
    columns = expert_input.shape[1]
    lanes = 128
    first = max(lanes, columns * 4 // 8 // lanes * lanes)
    spans = [(0, first), (first, columns - first)] if first < columns else [(0, columns)]
    dispatched = []
    for begin, span in spans:
        part = expert_input[:, begin : begin + span]
        buffer = jnp.dot(chosen, part, preferred_element_type=jnp.float32).astype(jnp.bfloat16)
        dispatched.append(send_out(buffer, expert_count))

    def added(sums, source, piece, begin):
        start, span = source * columns + begin, piece.shape[1]
        features = piece.astype(jnp.float32)
        gained = (features * rows_of(expert_gain, start, span)[None, :]).astype(jnp.bfloat16)
        parts = (
            jnp.dot(gained, rows_of(gate_block, start, span), preferred_element_type=jnp.float32),
            jnp.dot(gained, rows_of(up_block, start, span), preferred_element_type=jnp.float32),
            jnp.sum(features * features, axis=1),
        )
        return parts if sums is None else tuple(a + b for a, b in zip(sums, parts))

    sums = None
    later = []
    for number, (begin, span) in enumerate(spans):
        arrived = dispatched[number]
        if number > 0:
            arrived, sums = lax.optimization_barrier((arrived, sums))
        pieces = pieces_over_tp(arrived)
        for source, piece in pieces[:2]:
            sums = added(sums, source, piece, begin)
        later = later + [(source, piece, begin) for source, piece in pieces[2:]]
    for source, piece, begin in later:
        sums = added(sums, source, piece, begin)
    gate_sum, up_sum, squares = sums
    scale = lax.rsqrt(squares / D + EPS)[:, None]
    hidden = (jax.nn.silu(gate_sum * scale) * (up_sum * scale)).astype(jnp.bfloat16)
    results = summed_product(pieces_over_tp(hidden), down_block).astype(jnp.bfloat16)
    returned = send_back(results, expert_count)

    products = conv_in_gate.astype(jnp.float32) * conv_value.astype(jnp.float32)
    earlier_rows = shifted(products[token_rows - reach :], "ep", 1)
    padded = jnp.concatenate([earlier_rows, products], axis=0)
    convolved = jnp.zeros_like(products)
    for offset in range(reach + 1):
        convolved = convolved + conv_taps[offset][None, :] * padded[offset : offset + token_rows]
    mixer_rows = (conv_gate.astype(jnp.float32) * convolved).astype(jnp.bfloat16)
    mixed = summed_product(pieces_over_tp(mixer_rows), mix_out_weight).astype(jnp.bfloat16)

    weights = pair_weights(group_prob, pair_logits)
    by_expert = jnp.sum(member * weights[:, None, :], axis=2)
    spread_weights = (
        (place[:, :, None] == slot[None, None, :]).astype(jnp.float32) * by_expert[:, :, None]
    ).reshape(tok_rows, slot_rows)
    high = lax.reduce_precision(spread_weights, 8, 7)
    low = (spread_weights - high).astype(jnp.bfloat16)
    expert_output = (
        jnp.dot(high.astype(jnp.bfloat16), returned, preferred_element_type=jnp.float32)
        + jnp.dot(low, returned, preferred_element_type=jnp.float32)
    ).astype(jnp.bfloat16)
    return (mixed, expert_output)


def solution(mesh):
    in_specs = (
        P("ep", "tp"),
        P("ep", "tp"),
        P("ep", "tp"),
        P(None, "tp"),
        P(None, "tp"),
        P("ep", "tp"),
        P(),
        P("ep", None),
        P("ep"),
        P("ep", None),
        P("ep", None, "tp"),
        P("ep", None, "tp"),
        P("ep", None, "tp"),
    )
    out_specs = (P("ep", "tp"), P("ep", "tp"))
    return jax.shard_map(
        per_device, mesh=mesh, in_specs=in_specs, out_specs=out_specs, check_vma=False
    )
```
